256 devices in a mesh: grp: 2 (over y), sp: 16 (over z), tp: 8 (over x, core).
Axes of the slice: x: 4, y: 2, z: 16, core: 2. Of those that a mesh axis runs over, the one named last changes fastest.
The devices are a block of a 4x16x16 slice.
Arguments:
- layer_input: bfloat16 [64, 6144, 2048], P(('grp', 'tp'), 'sp'), parts along dimension 0, may hold values from -6 to 6
- input_gain: float32 [2048], replicated, may hold values from 0.1 to 1.9
- key_weight: bfloat16 [2048, 512], replicated, may hold values from -0.125 to 0.125
- value_weight: bfloat16 [2048, 512], replicated, may hold values from -0.125 to 0.125
- stick_offsets: bfloat16 [4, 64, 6144], P(None, ('grp', 'tp'), 'sp'), parts along dimension 1
- head_bias: float32 [16], replicated
- queries: bfloat16 [16, 16, 512], P(('grp', 'tp'), 'sp'), parts along dimension 0, may hold values from -6 to 6
Outputs:
- key_cache: bfloat16 [16, 16, 6144, 128], P(('grp', 'tp'), 'sp'), parts along dimension 0
- value_cache: bfloat16 [16, 16, 6144, 128], P(('grp', 'tp'), 'sp'), parts along dimension 0
- offset_cache: bfloat16 [16, 16, 6144], P(('grp', 'tp'), 'sp'), parts along dimension 0
- first_read: bfloat16 [16, 16, 512], P(('grp', 'tp'), 'sp'), parts along dimension 0
The draws below stay inside these ranges and needn't reach their ends.
There are 2 independent parts, one for each index of `grp`. The reference program is written for one: setup_inputs(seed, part) draws one part's arguments, and reference() takes and returns one part's arrays. A program takes and returns all parts, laid end to end along the dimension named above; an argument that names none is the same for every part. Nothing has to cross between parts.
All inputs are finite; a program needn't handle non-finite values.
Results may differ from the reference program's by a relative error of at most 0.014.
Values may be sent and summed in bfloat16 or wider, within the bound.
A program may use at most 64 MiB of HBM per device.

```python
import math
import jax
import jax.numpy as jnp
from jax import lax

D = 2048
H = 16
KVH = 4
HD = 128
BLOCK = 384
QG = 4
SEQS = 32
LEN = 6144
N_SP = 16
N_TP = 8


def draw_head_bias(key, part):
    pick_key = jax.random.fold_in(key, 11)
    slow_key = jax.random.fold_in(key, 12)
    fast_key = jax.random.fold_in(key, 13)
    fast_share = 0.5
    fast_heads = jax.random.bernoulli(pick_key, fast_share, (H,))
    slow_value = -math.log(LEN) - jax.random.uniform(slow_key, (H,), jnp.float32, 0.5, 1.5)
    fast_value = -4.0 + jax.random.uniform(fast_key, (H,), jnp.float32, -0.5, 0.5)
    return jnp.where(fast_heads, fast_value, slow_value).astype(jnp.float32)


def draw_stick_offsets(key, part):
    level_key = jax.random.fold_in(key, 21)
    jitter_key = jax.random.fold_in(key, 22)
    place_key = jax.random.fold_in(key, 23)
    height_key = jax.random.fold_in(key, 24)
    level_range = 0.7
    blocks = LEN // BLOCK
    tier_entries = jax.random.uniform(level_key, (KVH, SEQS, blocks), jnp.float32, -level_range, level_range)
    tier_entries = jnp.repeat(tier_entries, BLOCK, axis=2)
    stochastic_jitter = jnp.clip(0.3 * jax.random.normal(jitter_key, (KVH, SEQS, LEN), jnp.float32), -1.0, 1.0)
    slot_destinations = jax.random.randint(place_key, (KVH, SEQS, 2), 0, LEN)
    vertical_extent_entries = math.log(LEN) + jax.random.uniform(height_key, (KVH, SEQS, 2), jnp.float32, 0.0, 1.0)
    sequence_slot_index = jnp.arange(LEN)
    clustered_sets = jnp.sum(jnp.where(sequence_slot_index[None, None, None, :] == slot_destinations[..., None], vertical_extent_entries[..., None], 0.0), axis=2)
    return (tier_entries + stochastic_jitter + clustered_sets).astype(jnp.bfloat16)


def level_of(stream_key, shape, cuts, least, top_value):
    def one(position, blocks):
        steps = jax.random.uniform(jax.random.fold_in(jax.random.fold_in(stream_key, 6), position), (blocks,), jnp.float32, least / len(cuts), top_value / len(cuts))
        return jnp.repeat(jnp.exp(steps), shape[position] // blocks).reshape((-1,) + (1,) * (len(shape) - position - 1))

    loudness = one(*cuts[0])
    for cut in cuts[1:]:
        loudness = loudness * one(*cut)
    return loudness


def normal_values(stream_key, dims, scale, bound, split=(), held_as=jnp.bfloat16):
    entries = jax.random.normal(stream_key, dims, jnp.float32) * scale
    if len(split) > 0:
        entries = level_of(stream_key, dims, split, -0.22, 0.18) * entries
    return jnp.clip(entries, min=-bound, max=bound).astype(held_as)


def setup_inputs(seed: int = 0, part: int = 0) -> dict:
    seeds = jax.random.split(jax.random.key(seed), 8)
    part_splits = jax.random.split(jax.random.fold_in(seeds[7], part), 8)
    return {
        "layer_input": normal_values(part_splits[0], (SEQS, LEN, D), 1.0, 6.0, ((0, 8), (1, 16))),
        "input_gain": jnp.clip(1.0 + 0.18 * jax.random.normal(seeds[1], (D,), jnp.float32), 0.1, 1.9),
        "key_weight": normal_values(seeds[2], (D, KVH * HD), D ** -0.5, 0.125),
        "value_weight": normal_values(seeds[3], (D, KVH * HD), D ** -0.5, 0.125),
        "stick_offsets": draw_stick_offsets(jax.random.fold_in(jax.random.fold_in(seeds[7], part), 71), part),
        "head_bias": draw_head_bias(jax.random.fold_in(seeds[7], 71), part),
        "queries": normal_values(part_splits[6], (N_TP, N_SP, QG * HD), 1.0, 6.0, ((0, 8), (1, 16))),
    }


EPSILON = 1e-06

def rms_scale(matrix):
    return matrix * lax.rsqrt(lax.optimization_barrier(jnp.mean(matrix * matrix, axis=-1, keepdims=True)) + EPSILON)

def stick_weights(scores, spread, carried):
    inside = lax.cumsum(spread, axis=scores.ndim - 1, reverse=True) - spread
    return jnp.exp(jax.nn.log_sigmoid(scores) - inside - carried)

def reference(layer_input, input_gain, key_weight, value_weight, stick_offsets, head_bias, queries):
    group_size = H // KVH
    per_column = N_SP // KVH

    def one_sequence(tokens):
        widened = tokens.astype(jnp.float32)
        normed_rows = (rms_scale(widened) * input_gain).astype(jnp.bfloat16)
        key_rows = jnp.dot(normed_rows, key_weight, preferred_element_type=jnp.float32).astype(jnp.bfloat16)
        value_rows = jnp.dot(normed_rows, value_weight, preferred_element_type=jnp.float32).astype(jnp.bfloat16)
        return (key_rows, value_rows)
    key_rows, value_rows = lax.map(one_sequence, layer_input)
    key_cache = jnp.transpose(key_rows.reshape(N_TP, per_column, LEN, KVH, HD), (0, 1, 3, 2, 4)).reshape(N_TP, N_SP, LEN, HD)
    value_cache = jnp.transpose(value_rows.reshape(N_TP, per_column, LEN, KVH, HD), (0, 1, 3, 2, 4)).reshape(N_TP, N_SP, LEN, HD)
    offset_cache = jnp.transpose(stick_offsets.reshape(KVH, N_TP, per_column, LEN), (1, 2, 0, 3)).reshape(N_TP, N_SP, LEN)
    bias_all = jnp.tile(head_bias.reshape(KVH, group_size), (N_TP * per_column, 1))

    def one_read(pieces):
        query_row, key_block, value_block, offset_row, bias_row = pieces
        scores = jnp.dot(query_row.reshape(group_size, HD), key_block.T, preferred_element_type=jnp.float32)
        scores = scores / math.sqrt(HD) + bias_row[:, None] + offset_row.astype(jnp.float32)[None, :]
        spread = jax.nn.softplus(scores)
        weights = stick_weights(scores, spread, 0.0).astype(jnp.bfloat16)
        mixture = jnp.dot(weights, value_block, preferred_element_type=jnp.float32)
        return rms_scale(mixture).astype(jnp.bfloat16).reshape(group_size * HD)
    first_read = lax.map(one_read, (queries.reshape(N_TP * N_SP, group_size * HD), key_cache.reshape(N_TP * N_SP, LEN, HD), value_cache.reshape(N_TP * N_SP, LEN, HD), offset_cache.reshape(N_TP * N_SP, LEN), bias_all))
    return (key_cache, value_cache, offset_cache, first_read.reshape(N_TP, N_SP, group_size * HD))
```

```python
import functools
import math

import jax
import jax.numpy as jnp
from jax import lax
from jax.experimental import pallas as pl
from jax.experimental.pallas import tpu as pltpu
from jax.sharding import PartitionSpec as P

H = 16
KVH = 4
HD = 128
EPSILON = 1e-06
MESH = pl.DeviceIdType.MESH
NORM_ROWS = 16


def split_rows(row, count):
    return [row[:, k * HD : (k + 1) * HD] for k in range(count)]


def kernel(
    n,
    x_ref, gain_ref, wk_ref, wv_ref, off_ref, bias_ref, q_ref,
    key_ref, value_ref, off_out_ref, read_ref,
    x_buf, w_buf, normed, sent, held, off_sent, off_held, later, mixes, totals,
    x_sem, w_sem, send_sem, recv_sem, off_send_sem, off_recv_sem, out_sem, chain, ready,
):
    prompts, block, _ = x_ref.shape
    group = H // KVH
    lane_rows = block // HD
    me = lax.axis_index("sp")
    barrier = pltpu.get_barrier_semaphore()
    pl.semaphore_signal(barrier, inc=1, device_id={"sp": lax.rem(me + n - 1, n)}, device_id_type=MESH)

    def x_copy(i):
        return pltpu.make_async_copy(x_ref.at[i], x_buf.at[i], x_sem.at[i])

    def w_copies(h):
        columns = pl.ds(h * HD, HD)
        return (
            pltpu.make_async_copy(wk_ref.at[:, columns], w_buf.at[h, :, pl.ds(0, HD)], w_sem.at[h, 0]),
            pltpu.make_async_copy(wv_ref.at[:, columns], w_buf.at[h, :, pl.ds(HD, HD)], w_sem.at[h, 1]),
        )

    x_copy(0).start()
    for h in range(KVH):
        for copy in w_copies(h):
            copy.start()
    for i in range(1, prompts):
        x_copy(i).start()

    for h in range(KVH):
        rows = off_ref[h].astype(jnp.float32)
        for i in range(prompts):
            pieces = split_rows(rows[i : i + 1], lane_rows)
            off_sent[i * KVH + h] = jnp.concatenate(pieces + pieces[:1], axis=0).astype(jnp.bfloat16)
    below = lax.broadcasted_iota(jnp.int32, (block, block), 0)
    across = lax.broadcasted_iota(jnp.int32, (block, block), 1)
    later[...] = jnp.where(below > across, 1.0, 0.0).astype(jnp.bfloat16)

    pl.semaphore_wait(barrier, 1)

    @pl.when(me > 0)
    def _():
        pl.semaphore_wait(chain, 1)

    def announce(t, carry):
        pl.semaphore_signal(ready.at[me], inc=1, device_id={"sp": t}, device_id_type=MESH)
        return carry

    lax.fori_loop(0, me, announce, 0)

    @pl.when(me < n - 1)
    def _():
        pl.semaphore_signal(chain, inc=1, device_id={"sp": lax.rem(me + 1, n)}, device_id_type=MESH)

    def copies(t, slot):
        to = {"sp": t}
        return (
            pltpu.make_async_remote_copy(
                sent.at[t, 0], held.at[slot, 0], send_sem.at[t, 0], recv_sem.at[slot, 0], device_id=to, device_id_type=MESH
            ),
            pltpu.make_async_remote_copy(
                sent.at[t, 1], held.at[slot, 1], send_sem.at[t, 1], recv_sem.at[slot, 1], device_id=to, device_id_type=MESH
            ),
            pltpu.make_async_remote_copy(
                off_sent.at[t], off_held.at[slot], off_send_sem.at[t], off_recv_sem.at[slot], device_id=to, device_id_type=MESH
            ),
        )

    def send(t):
        for copy in copies(t, me):
            copy.start()

    def project_prompt(i, carry):
        x_copy(i).wait()

        def norm(r, carry):
            rows = pl.ds(pl.multiple_of(r * NORM_ROWS, NORM_ROWS), NORM_ROWS)
            x = x_buf[i, rows, :].astype(jnp.float32)
            scale = lax.rsqrt(jnp.mean(x * x, axis=-1, keepdims=True) + EPSILON)
            normed[rows, :] = (x * scale * gain_ref[...]).astype(jnp.bfloat16)
            return carry

        lax.fori_loop(0, block // NORM_ROWS, norm, 0)

        def project_head(h, carry):
            t = i * KVH + h

            @pl.when(i == 0)
            def _():
                for copy in w_copies(h):
                    copy.wait()

            rows = jnp.dot(normed[...], w_buf[h], preferred_element_type=jnp.float32).astype(jnp.bfloat16)

            @pl.when(t != me)
            def _():
                sent[t, 0] = rows[:, :HD]
                sent[t, 1] = rows[:, HD:]

            @pl.when(t == me)
            def _():
                held[me, 0] = rows[:, :HD]
                held[me, 1] = rows[:, HD:]
                off_held[me] = off_sent[t]

            @pl.when(jnp.logical_and(t >= 1, t - 1 < me))
            def _():
                send(t - 1)

            return carry

        lax.fori_loop(0, KVH, project_head, 0)
        return carry

    lax.fori_loop(0, prompts, project_prompt, 0)

    def send_later(t, carry):
        pl.semaphore_wait(ready.at[t], 1)
        send(t)
        return carry

    lax.fori_loop(me + 1, n, send_later, 0)

    head = lax.rem(me, KVH)
    row_index = lax.broadcasted_iota(jnp.int32, (2 * group, 1), 0)
    query_rows = split_rows(q_ref[0], group)
    query = jnp.concatenate(query_rows + query_rows, axis=0)
    bias = jnp.zeros((2 * group, 1), jnp.float32)
    for g in range(group):
        bias = jnp.where(lax.rem(row_index, group) == g, bias_ref[head * group + g], bias)

    def out_copies(slot):
        rows = pl.ds(pl.multiple_of(slot * block, block), block)
        return (
            pltpu.make_async_copy(held.at[slot, 0], key_ref.at[0, 0, rows, :], out_sem.at[slot, 0]),
            pltpu.make_async_copy(held.at[slot, 1], value_ref.at[0, 0, rows, :], out_sem.at[slot, 1]),
        )

    def read_block(j, carry):
        slot = lax.rem(me + j, n)

        @pl.when(j > 0)
        def _():
            for copy in copies(slot, slot):
                copy.wait_recv()

        for copy in out_copies(slot):
            copy.start()
        off_rows = off_held[slot].astype(jnp.float32)
        off_row = jnp.concatenate([off_rows[k : k + 1] for k in range(lane_rows)], axis=1)
        off_out_ref[0, :, pl.ds(pl.multiple_of(slot * block, HD), block)] = off_row.astype(jnp.bfloat16)
        scores = lax.dot_general(query, held[slot, 0], (((1,), (1,)), ((), ())), preferred_element_type=jnp.float32)
        scores = scores * (1.0 / math.sqrt(HD)) + bias + off_row
        tail = jnp.log1p(jnp.exp(-jnp.abs(scores)))
        spread = jnp.maximum(scores, 0.0) + tail
        log_take = jnp.minimum(scores, 0.0) - tail
        high = spread.astype(jnp.bfloat16)
        rest = spread - high.astype(jnp.float32)
        middle = rest.astype(jnp.bfloat16)
        low = (rest - middle.astype(jnp.float32)).astype(jnp.bfloat16)
        inside = (
            jnp.dot(high, later[...], preferred_element_type=jnp.float32)
            + jnp.dot(middle, later[...], preferred_element_type=jnp.float32)
            + jnp.dot(low, later[...], preferred_element_type=jnp.float32)
        )
        weights = jnp.exp(log_take - inside)
        coarse = weights.astype(jnp.bfloat16)
        fine = (weights - coarse.astype(jnp.float32)).astype(jnp.bfloat16)
        both = jnp.where(row_index < group, coarse.astype(jnp.float32), fine.astype(jnp.float32)).astype(jnp.bfloat16)
        mixes[slot] = jnp.dot(both, held[slot, 1], preferred_element_type=jnp.float32)
        totals[slot] = jnp.broadcast_to(jnp.sum(spread, axis=-1, keepdims=True), (2 * group, HD))
        return carry

    lax.fori_loop(0, n, read_block, 0)

    def fold(j, carry):
        mixture, beyond = carry
        slot = n - 1 - j
        return mixture + jnp.exp(-beyond) * mixes[slot], beyond + totals[slot]

    zeros = jnp.zeros((2 * group, HD), jnp.float32)
    mixture, _ = lax.fori_loop(0, n, fold, (zeros, zeros))
    mixture = mixture[:group] + mixture[group:]
    mixture = mixture * lax.rsqrt(jnp.mean(mixture * mixture, axis=-1, keepdims=True) + EPSILON)
    read_ref[0] = jnp.concatenate([mixture[g : g + 1] for g in range(group)], axis=1).astype(jnp.bfloat16)

    def finish(j, carry):
        slot = lax.rem(me + j, n)

        @pl.when(j > 0)
        def _():
            for copy in copies(slot, slot):
                copy.wait_send()

        for copy in out_copies(slot):
            copy.wait()
        return carry

    lax.fori_loop(0, n, finish, 0)


def shards(layer_input, input_gain, key_weight, value_weight, stick_offsets, head_bias, queries):
    seq_count, block, width = layer_input.shape
    n = lax.axis_size("sp")
    length = n * block
    group = H // KVH
    hbm = pl.BlockSpec(memory_space=pl.ANY)
    vmem = pl.BlockSpec(memory_space=pltpu.VMEM)
    smem = pl.BlockSpec(memory_space=pltpu.SMEM)
    return pl.pallas_call(
        functools.partial(kernel, n),
        out_shape=(
            jax.ShapeDtypeStruct((1, 1, length, HD), jnp.bfloat16),
            jax.ShapeDtypeStruct((1, 1, length, HD), jnp.bfloat16),
            jax.ShapeDtypeStruct((1, 1, length), jnp.bfloat16),
            jax.ShapeDtypeStruct((1, 1, group * HD), jnp.bfloat16),
        ),
        in_specs=[hbm, vmem, hbm, hbm, vmem, smem, vmem],
        out_specs=(hbm, hbm, vmem, vmem),
        scratch_shapes=[
            pltpu.VMEM((seq_count, block, width), jnp.bfloat16),
            pltpu.VMEM((KVH, width, 2 * HD), jnp.bfloat16),
            pltpu.VMEM((block, width), jnp.bfloat16),
            pltpu.VMEM((n, 2, block, HD), jnp.bfloat16),
            pltpu.VMEM((n, 2, block, HD), jnp.bfloat16),
            pltpu.VMEM((n, 4, HD), jnp.bfloat16),
            pltpu.VMEM((n, 4, HD), jnp.bfloat16),
            pltpu.VMEM((block, block), jnp.bfloat16),
            pltpu.VMEM((n, 2 * group, HD), jnp.float32),
            pltpu.VMEM((n, 2 * group, HD), jnp.float32),
            pltpu.SemaphoreType.DMA((seq_count,)),
            pltpu.SemaphoreType.DMA((KVH, 2)),
            pltpu.SemaphoreType.DMA((n, 2)),
            pltpu.SemaphoreType.DMA((n, 2)),
            pltpu.SemaphoreType.DMA((n,)),
            pltpu.SemaphoreType.DMA((n,)),
            pltpu.SemaphoreType.DMA((n, 2)),
            pltpu.SemaphoreType.REGULAR,
            pltpu.SemaphoreType.REGULAR((n,)),
        ],
        compiler_params=pltpu.CompilerParams(collective_id=0, has_side_effects=True),
    )(
        layer_input,
        input_gain.reshape(1, width),
        key_weight,
        value_weight,
        stick_offsets,
        head_bias,
        queries,
    )


def solution(mesh):
    placed = (
        P(("grp", "tp"), "sp", None),
        P(),
        P(),
        P(),
        P(None, ("grp", "tp"), "sp"),
        P(),
        P(("grp", "tp"), "sp", None),
    )
    return jax.shard_map(
        shards,
        mesh=mesh,
        in_specs=placed,
        out_specs=(
            P(("grp", "tp"), "sp", None, None),
            P(("grp", "tp"), "sp", None, None),
            P(("grp", "tp"), "sp", None),
            P(("grp", "tp"), "sp", None),
        ),
        check_vma=False,
    )
```

```python
import functools
import math

import jax
import jax.numpy as jnp
from jax import lax
from jax.experimental import pallas as pl
from jax.experimental.pallas import tpu as pltpu
from jax.sharding import PartitionSpec as P

H = 16
KVH = 4
HD = 128
EPSILON = 1e-06
MESH = pl.DeviceIdType.MESH
NORM_ROWS = 16
VMEM_LIMIT = 40 * 2**20


def split_rows(row, count):
    return [row[:, k * HD : (k + 1) * HD] for k in range(count)]


def kernel(
    n,
    x_ref, gain_hbm, wk_ref, wv_ref, off_hbm, bias_hbm, q_hbm,
    key_ref, value_ref, off_out_ref, read_ref,
    gain_ref, off_ref, bias_ref, q_ref, small_sem, x_buf, w_buf, normed, sent, relayed, off_sent, off_held, later, mixes, totals,
    x_sem, w_sem, send_sem, recv_sem, off_send_sem, off_recv_sem, relay_send_sem, relay_recv_sem, ready,
):
    prompts, block, _ = x_ref.shape
    group = H // KVH
    lane_rows = block // HD
    me = lax.axis_index("sp")
    barrier = pltpu.get_barrier_semaphore()

    def x_copy(i):
        return pltpu.make_async_copy(x_ref.at[i], x_buf.at[i], x_sem.at[i])

    def w_copies(h):
        columns = pl.ds(h * HD, HD)
        return (
            pltpu.make_async_copy(wk_ref.at[:, columns], w_buf.at[h, :, pl.ds(0, HD)], w_sem.at[h, 0]),
            pltpu.make_async_copy(wv_ref.at[:, columns], w_buf.at[h, :, pl.ds(HD, HD)], w_sem.at[h, 1]),
        )

    small = [
        pltpu.make_async_copy(source, target, small_sem.at[k])
        for k, (source, target) in enumerate(
            ((off_hbm, off_ref), (gain_hbm, gain_ref), (bias_hbm, bias_ref), (q_hbm, q_ref))
        )
    ]
    x_copy(0).start()
    for copy in small:
        copy.start()
    for h in range(KVH):
        for copy in w_copies(h):
            copy.start()
    for i in range(1, prompts):
        x_copy(i).start()

    @pl.when(me > 0)
    def _():
        pl.semaphore_wait(barrier, 1)

    @pl.when(me < n - 1)
    def _():
        pl.semaphore_signal(barrier, inc=1, device_id={"sp": lax.rem(me + 1, n)}, device_id_type=MESH)

    def announce(t, carry):
        pl.semaphore_signal(ready.at[me], inc=1, device_id={"sp": t}, device_id_type=MESH)
        return carry

    lax.fori_loop(0, me, announce, 0)

    for copy in small:
        copy.wait()
    for h in range(KVH):
        rows = off_ref[h].astype(jnp.float32)
        for i in range(prompts):
            pieces = split_rows(rows[i : i + 1], lane_rows)
            off_sent[i * KVH + h] = jnp.concatenate(pieces + pieces[:1], axis=0).astype(jnp.bfloat16)

    half, quarter = n // 2, n // 4
    from_low = jnp.logical_and(me < quarter, lax.rem(me, 2) == 1)
    from_high = jnp.logical_and(me >= n - quarter, lax.rem(me, 2) == 0)
    relays_low = jnp.logical_and(jnp.logical_and(me >= quarter, me < half), lax.rem(me, 2) == 1)
    relays_high = jnp.logical_and(jnp.logical_and(me >= half, me < n - quarter), lax.rem(me, 2) == 0)
    by_relay = jnp.logical_or(from_low, from_high)
    relays = jnp.logical_or(relays_low, relays_high)
    opposite = lax.rem(me + half, n)
    step = jnp.where(me < half, quarter, n - quarter)
    onward = lax.rem(me + step, n)
    origin = lax.rem(me - step + n, n)

    caches = (key_ref, value_ref)

    def place(kv, slot):
        return caches[kv].at[0, 0, pl.ds(pl.multiple_of(slot * block, block), block), :]

    def block_copy(kv, t, slot):
        return pltpu.make_async_remote_copy(
            sent.at[t, kv], place(kv, slot), send_sem.at[t, kv], recv_sem.at[slot, kv], device_id={"sp": t}, device_id_type=MESH
        )

    def off_copy(t, slot):
        return pltpu.make_async_remote_copy(
            off_sent.at[t], off_held.at[slot], off_send_sem.at[t], off_recv_sem.at[slot], device_id={"sp": t}, device_id_type=MESH
        )

    def relay_copy(kv):
        return pltpu.make_async_remote_copy(
            sent.at[opposite, kv], relayed.at[kv], send_sem.at[opposite, kv], relay_recv_sem.at[kv],
            device_id={"sp": onward}, device_id_type=MESH,
        )

    def onward_copy(kv):
        return pltpu.make_async_remote_copy(
            relayed.at[kv], place(kv, origin), relay_send_sem.at[kv], recv_sem.at[origin, kv],
            device_id={"sp": onward}, device_id_type=MESH,
        )

    def send(t):
        off_copy(t, me).start()
        through = jnp.logical_and(by_relay, t == opposite)

        @pl.when(through)
        def _():
            for kv in range(2):
                relay_copy(kv).start()

        @pl.when(jnp.logical_not(through))
        def _():
            for kv in range(2):
                block_copy(kv, t, me).start()

    def project_prompt(i, carry):
        x_copy(i).wait()

        def norm(r, carry):
            rows = pl.ds(pl.multiple_of(r * NORM_ROWS, NORM_ROWS), NORM_ROWS)
            x = x_buf[i, rows, :].astype(jnp.float32)
            scale = lax.rsqrt(jnp.mean(x * x, axis=-1, keepdims=True) + EPSILON)
            normed[rows, :] = (x * scale * gain_ref[...]).astype(jnp.bfloat16)
            return carry

        lax.fori_loop(0, block // NORM_ROWS, norm, 0)

        def project_head(h, carry):
            t = i * KVH + h

            @pl.when(i == 0)
            def _():
                for copy in w_copies(h):
                    copy.wait()

            rows = jnp.dot(normed[...], w_buf[h], preferred_element_type=jnp.float32).astype(jnp.bfloat16)

            @pl.when(t != me)
            def _():
                sent[t, 0] = rows[:, :HD]
                sent[t, 1] = rows[:, HD:]

            @pl.when(t == me)
            def _():
                own = pl.ds(pl.multiple_of(me * block, block), block)
                key_ref[0, 0, own, :] = rows[:, :HD]
                value_ref[0, 0, own, :] = rows[:, HD:]
                off_held[me] = off_sent[t]

            @pl.when(jnp.logical_and(t >= 1, t - 1 < me))
            def _():
                send(t - 1)

            return carry

        lax.fori_loop(0, KVH, project_head, 0)
        return carry

    lax.fori_loop(0, prompts, project_prompt, 0)

    def send_later(t, carry):
        pl.semaphore_wait(ready.at[t], 1)
        send(t)
        return carry

    lax.fori_loop(me + 1, n, send_later, 0)

    @pl.when(relays)
    def _():
        for kv in range(2):
            relay_copy(kv).wait_recv()
            onward_copy(kv).start()

    below = lax.broadcasted_iota(jnp.int32, (block, block), 0)
    across = lax.broadcasted_iota(jnp.int32, (block, block), 1)
    later[...] = jnp.where(below > across, 1.0, 0.0).astype(jnp.bfloat16)

    head = lax.rem(me, KVH)
    row_index = lax.broadcasted_iota(jnp.int32, (2 * group, 1), 0)
    query_rows = split_rows(q_ref[0], group)
    query = jnp.concatenate(query_rows + query_rows, axis=0)
    bias = jnp.zeros((2 * group, 1), jnp.float32)
    for g in range(group):
        bias = jnp.where(lax.rem(row_index, group) == g, bias_ref[head * group + g], bias)

    def read_block(j, carry):
        slot = lax.rem(me + j, n)

        @pl.when(j > 0)
        def _():
            off_copy(slot, slot).wait_recv()
            for kv in range(2):
                block_copy(kv, slot, slot).wait_recv()

        rows = pl.ds(pl.multiple_of(slot * block, block), block)
        off_rows = off_held[slot].astype(jnp.float32)
        off_row = jnp.concatenate([off_rows[k : k + 1] for k in range(lane_rows)], axis=1)
        off_out_ref[0, :, pl.ds(pl.multiple_of(slot * block, HD), block)] = off_row.astype(jnp.bfloat16)
        scores = lax.dot_general(query, key_ref[0, 0, rows, :], (((1,), (1,)), ((), ())), preferred_element_type=jnp.float32)
        scores = scores * (1.0 / math.sqrt(HD)) + bias + off_row
        tail = jnp.log1p(jnp.exp(-jnp.abs(scores)))
        spread = jnp.maximum(scores, 0.0) + tail
        log_take = jnp.minimum(scores, 0.0) - tail
        high = spread.astype(jnp.bfloat16)
        rest = spread - high.astype(jnp.float32)
        middle = rest.astype(jnp.bfloat16)
        low = (rest - middle.astype(jnp.float32)).astype(jnp.bfloat16)
        inside = (
            jnp.dot(high, later[...], preferred_element_type=jnp.float32)
            + jnp.dot(middle, later[...], preferred_element_type=jnp.float32)
            + jnp.dot(low, later[...], preferred_element_type=jnp.float32)
        )
        weights = jnp.exp(log_take - inside)
        coarse = weights.astype(jnp.bfloat16)
        fine = (weights - coarse.astype(jnp.float32)).astype(jnp.bfloat16)
        both = jnp.where(row_index < group, coarse.astype(jnp.float32), fine.astype(jnp.float32)).astype(jnp.bfloat16)
        mixes[slot] = jnp.dot(both, value_ref[0, 0, rows, :], preferred_element_type=jnp.float32)
        totals[slot] = jnp.broadcast_to(jnp.sum(spread, axis=-1, keepdims=True), (2 * group, HD))
        return carry

    lax.fori_loop(0, n, read_block, 0)

    def fold(j, carry):
        mixture, beyond = carry
        slot = n - 1 - j
        return mixture + jnp.exp(-beyond) * mixes[slot], beyond + totals[slot]

    zeros = jnp.zeros((2 * group, HD), jnp.float32)
    mixture, _ = lax.fori_loop(0, n, fold, (zeros, zeros))
    mixture = mixture[:group] + mixture[group:]
    mixture = mixture * lax.rsqrt(jnp.mean(mixture * mixture, axis=-1, keepdims=True) + EPSILON)
    read_ref[0] = jnp.concatenate([mixture[g : g + 1] for g in range(group)], axis=1).astype(jnp.bfloat16)

    def finish(j, carry):
        slot = lax.rem(me + j, n)

        @pl.when(j > 0)
        def _():
            off_copy(slot, slot).wait_send()
            for kv in range(2):
                block_copy(kv, slot, slot).wait_send()

        return carry

    lax.fori_loop(0, n, finish, 0)

    @pl.when(relays)
    def _():
        for kv in range(2):
            onward_copy(kv).wait_send()


def store_kernel(key_ref, value_ref, off_ref, read_ref, key_out, value_out, off_out, read_out, sems):
    copies = [
        pltpu.make_async_copy(source, target, sems.at[k])
        for k, (source, target) in enumerate(
            ((key_ref, key_out), (value_ref, value_out), (off_ref, off_out), (read_ref, read_out))
        )
    ]
    for copy in copies:
        copy.start()
    for copy in copies:
        copy.wait()


def shards(layer_input, input_gain, key_weight, value_weight, stick_offsets, head_bias, queries):
    seq_count, block, width = layer_input.shape
    n = lax.axis_size("sp")
    length = n * block
    group = H // KVH
    hbm = pl.BlockSpec(memory_space=pl.ANY)
    vmem = pl.BlockSpec(memory_space=pltpu.VMEM)
    smem = pl.BlockSpec(memory_space=pltpu.SMEM)
    shapes = ((1, 1, length, HD), (1, 1, length, HD), (1, 1, length), (1, 1, group * HD))
    arrived = pl.pallas_call(
        functools.partial(kernel, n),
        out_shape=tuple(pltpu.VMEM(shape, jnp.bfloat16) for shape in shapes),
        in_specs=[hbm] * 7,
        out_specs=(vmem, vmem, vmem, vmem),
        scratch_shapes=[
            pltpu.VMEM((1, width), jnp.float32),
            pltpu.VMEM(stick_offsets.shape, jnp.bfloat16),
            pltpu.SMEM(head_bias.shape, jnp.float32),
            pltpu.VMEM(queries.shape, jnp.bfloat16),
            pltpu.SemaphoreType.DMA((4,)),
            pltpu.VMEM((seq_count, block, width), jnp.bfloat16),
            pltpu.VMEM((KVH, width, 2 * HD), jnp.bfloat16),
            pltpu.VMEM((block, width), jnp.bfloat16),
            pltpu.VMEM((n, 2, block, HD), jnp.bfloat16),
            pltpu.VMEM((2, block, HD), jnp.bfloat16),
            pltpu.VMEM((n, 4, HD), jnp.bfloat16),
            pltpu.VMEM((n, 4, HD), jnp.bfloat16),
            pltpu.VMEM((block, block), jnp.bfloat16),
            pltpu.VMEM((n, 2 * group, HD), jnp.float32),
            pltpu.VMEM((n, 2 * group, HD), jnp.float32),
            pltpu.SemaphoreType.DMA((seq_count,)),
            pltpu.SemaphoreType.DMA((KVH, 2)),
            pltpu.SemaphoreType.DMA((n, 2)),
            pltpu.SemaphoreType.DMA((n, 2)),
            pltpu.SemaphoreType.DMA((n,)),
            pltpu.SemaphoreType.DMA((n,)),
            pltpu.SemaphoreType.DMA((2,)),
            pltpu.SemaphoreType.DMA((2,)),
            pltpu.SemaphoreType.REGULAR((n,)),
        ],
        compiler_params=pltpu.CompilerParams(collective_id=0, has_side_effects=True, vmem_limit_bytes=VMEM_LIMIT),
    )(
        *(
            pltpu.with_memory_space_constraint(array, pltpu.HBM)
            for array in (layer_input, input_gain.reshape(1, width), key_weight, value_weight, stick_offsets, head_bias, queries)
        )
    )
    return pl.pallas_call(
        store_kernel,
        out_shape=tuple(jax.ShapeDtypeStruct(shape, jnp.bfloat16) for shape in shapes),
        in_specs=[vmem] * 4,
        out_specs=(hbm,) * 4,
        scratch_shapes=[pltpu.SemaphoreType.DMA((4,))],
        compiler_params=pltpu.CompilerParams(vmem_limit_bytes=2**20),
    )(*arrived)


def solution(mesh):
    placed = (
        P(("grp", "tp"), "sp", None),
        P(),
        P(),
        P(),
        P(None, ("grp", "tp"), "sp"),
        P(),
        P(("grp", "tp"), "sp", None),
    )
    return jax.shard_map(
        shards,
        mesh=mesh,
        in_specs=placed,
        out_specs=(
            P(("grp", "tp"), "sp", None, None),
            P(("grp", "tp"), "sp", None, None),
            P(("grp", "tp"), "sp", None),
            P(("grp", "tp"), "sp", None),
        ),
        check_vma=False,
    )
```

```python
import functools
import math

import jax
import jax.numpy as jnp
from jax import lax
from jax.experimental import pallas as pl
from jax.experimental.pallas import tpu as pltpu
from jax.sharding import PartitionSpec as P

H = 16
KVH = 4
HD = 128
EPSILON = 1e-06
MESH = pl.DeviceIdType.MESH
NORM_ROWS = 128
FOLD_ROWS = 256
TIE_TURN = 11
VMEM_LIMIT = 40 * 2**20


def split_rows(row, count):
    return [row[:, k * HD : (k + 1) * HD] for k in range(count)]


def kernel(
    n,
    x_ref, gain_hbm, wk_ref, wv_ref, off_hbm, bias_hbm, q_hbm,
    key_ref, value_ref, off_out_ref, read_ref,
    gain_ref, off_ref, bias_ref, q_ref, small_sem, x_buf, w_in, w_buf, gain_rows, scales, sent, off_sent, off_held, later, mixes, totals,
    x_sem, w_sem, send_sem, recv_sem, off_send_sem, off_recv_sem, ready,
):
    prompts, block, width = x_ref.shape
    group = H // KVH
    lane_rows = block // HD
    me = lax.axis_index("sp")
    barrier = pltpu.get_barrier_semaphore()

    def x_copy(i):
        return pltpu.make_async_copy(x_ref.at[i], x_buf.at[i], x_sem.at[i])

    def w_copies(h):
        columns = pl.ds(h * HD, HD)
        return (
            pltpu.make_async_copy(wk_ref.at[:, columns], w_in.at[h, :, pl.ds(0, HD)], w_sem.at[h, 0]),
            pltpu.make_async_copy(wv_ref.at[:, columns], w_in.at[h, :, pl.ds(HD, HD)], w_sem.at[h, 1]),
        )

    small = [
        pltpu.make_async_copy(source, target, small_sem.at[k])
        for k, (source, target) in enumerate(
            ((off_hbm, off_ref), (gain_hbm, gain_ref), (bias_hbm, bias_ref), (q_hbm, q_ref))
        )
    ]
    x_copy(0).start()
    for copy in small:
        copy.start()
    for h in range(KVH):
        for copy in w_copies(h):
            copy.start()
    for i in range(1, prompts):
        x_copy(i).start()

    @pl.when(me > 0)
    def _():
        pl.semaphore_wait(barrier, 1)

    @pl.when(me < n - 1)
    def _():
        pl.semaphore_signal(barrier, inc=1, device_id={"sp": lax.rem(me + 1, n)}, device_id_type=MESH)

    def announce(t, carry):
        pl.semaphore_signal(ready.at[me], inc=1, device_id={"sp": t}, device_id_type=MESH)
        return carry

    lax.fori_loop(0, me, announce, 0)

    for copy in small:
        copy.wait()
    for k in range(width // HD):
        columns = jnp.broadcast_to(gain_ref[:, k * HD : (k + 1) * HD], (HD, HD))
        gain_rows[k * HD : (k + 1) * HD, :] = columns.T
    for h in range(KVH):
        rows = off_ref[h].astype(jnp.float32)
        for i in range(prompts):
            pieces = split_rows(rows[i : i + 1], lane_rows)
            off_sent[i * KVH + h] = jnp.concatenate(pieces + pieces[:1], axis=0).astype(jnp.bfloat16)

    half = n // 2
    caches = (key_ref, value_ref)

    def place(kv, slot):
        return caches[kv].at[0, 0, pl.ds(pl.multiple_of(slot * block, block), block), :]

    def block_copy(kv, t, slot):
        return pltpu.make_async_remote_copy(
            sent.at[t, kv], place(kv, slot), send_sem.at[t, kv], recv_sem.at[slot, kv], device_id={"sp": t}, device_id_type=MESH
        )

    def off_copy(t, slot):
        return pltpu.make_async_remote_copy(
            off_sent.at[t], off_held.at[slot], off_send_sem.at[t], off_recv_sem.at[slot], device_id={"sp": t}, device_id_type=MESH
        )

    def send(t):
        off_copy(t, me).start()
        for kv in range(2):
            block_copy(kv, t, me).start()

    def fold_gain(h):
        for copy in w_copies(h):
            copy.wait()

        def fold_rows(r, carry):
            rows = pl.ds(pl.multiple_of(r * FOLD_ROWS, FOLD_ROWS), FOLD_ROWS)
            gain = gain_rows[rows, :]
            for kv in range(2):
                columns = pl.ds(kv * HD, HD)
                w_buf[h, rows, columns] = (w_in[h, rows, columns].astype(jnp.float32) * gain).astype(jnp.bfloat16)
            return carry

        lax.fori_loop(0, width // FOLD_ROWS, fold_rows, 0)

    def measure_rows(i):
        x_copy(i).wait()

        def measure(r, carry):
            rows = pl.ds(pl.multiple_of(r * NORM_ROWS, NORM_ROWS), NORM_ROWS)
            squares = jnp.zeros((NORM_ROWS, HD), jnp.float32)
            for k in range(width // HD):
                x = x_buf[i, rows, pl.ds(k * HD, HD)].astype(jnp.float32)
                squares += x * x
            mean = jnp.sum(squares, axis=-1, keepdims=True) * (1.0 / width)
            scales[rows, :] = jnp.broadcast_to(lax.rsqrt(mean + EPSILON), (NORM_ROWS, HD))
            return carry

        lax.fori_loop(0, block // NORM_ROWS, measure, 0)

    def project_prompt(i, carry):
        measure_rows(i)

        def project_head(h, carry):
            t = i * KVH + h

            @pl.when(i == 0)
            def _():
                fold_gain(h)

            rows = jnp.dot(x_buf[i], w_buf[h], preferred_element_type=jnp.float32)
            scale = scales[...]
            keys = (rows[:, :HD] * scale).astype(jnp.bfloat16)
            values = (rows[:, HD:] * scale).astype(jnp.bfloat16)

            @pl.when(t != me)
            def _():
                sent[t, 0] = keys
                sent[t, 1] = values

            @pl.when(t == me)
            def _():
                own = pl.ds(pl.multiple_of(me * block, block), block)
                key_ref[0, 0, own, :] = keys
                value_ref[0, 0, own, :] = values
                off_held[me] = off_sent[t]

            @pl.when(t < me)
            def _():
                send(t)

            return carry

        lax.fori_loop(0, KVH, project_head, 0)
        return carry

    lax.fori_loop(0, prompts, project_prompt, 0)

    def send_later(t, carry):
        pl.semaphore_wait(ready.at[t], 1)
        send(t)
        return carry

    lax.fori_loop(me + 1, n, send_later, 0)

    below = lax.broadcasted_iota(jnp.int32, (block, block), 0)
    across = lax.broadcasted_iota(jnp.int32, (block, block), 1)
    later[...] = jnp.where(below > across, 1.0, 0.0).astype(jnp.bfloat16)

    head = lax.rem(me, KVH)
    row_index = lax.broadcasted_iota(jnp.int32, (2 * group, 1), 0)
    query_rows = split_rows(q_ref[0], group)
    query = jnp.concatenate(query_rows + query_rows, axis=0)
    bias = jnp.zeros((2 * group, 1), jnp.float32)
    for g in range(group):
        bias = jnp.where(lax.rem(row_index, group) == g, bias_ref[head * group + g], bias)

    def source(j):
        k = jnp.where(j > TIE_TURN, j - 2, j - 1)
        away = jnp.where(lax.rem(k, 2) == 0, half - 1 - k // 2, n - 1 - k // 2)
        away = jnp.where(j == TIE_TURN, half, away)
        return lax.rem(me + jnp.where(j == 0, 0, away), n)

    def read_block(j, carry):
        slot = source(j)

        @pl.when(j > 0)
        def _():
            off_copy(slot, slot).wait_recv()
            for kv in range(2):
                block_copy(kv, slot, slot).wait_recv()

        rows = pl.ds(pl.multiple_of(slot * block, block), block)
        off_rows = off_held[slot].astype(jnp.float32)
        off_row = jnp.concatenate([off_rows[k : k + 1] for k in range(lane_rows)], axis=1)
        off_out_ref[0, :, pl.ds(pl.multiple_of(slot * block, HD), block)] = off_row.astype(jnp.bfloat16)
        scores = lax.dot_general(query, key_ref[0, 0, rows, :], (((1,), (1,)), ((), ())), preferred_element_type=jnp.float32)
        scores = scores * (1.0 / math.sqrt(HD)) + bias + off_row
        tail = jnp.log1p(jnp.exp(-jnp.abs(scores)))
        spread = jnp.maximum(scores, 0.0) + tail
        log_take = jnp.minimum(scores, 0.0) - tail
        high = spread.astype(jnp.bfloat16)
        rest = spread - high.astype(jnp.float32)
        middle = rest.astype(jnp.bfloat16)
        low = (rest - middle.astype(jnp.float32)).astype(jnp.bfloat16)
        parts = jnp.concatenate([part.astype(jnp.float32) for part in (high, middle, low)], axis=0).astype(jnp.bfloat16)
        sums = jnp.dot(parts, later[...], preferred_element_type=jnp.float32)
        inside = sums[: 2 * group] + sums[2 * group : 4 * group] + sums[4 * group :]
        weights = jnp.exp(log_take - inside)
        coarse = weights.astype(jnp.bfloat16)
        fine = (weights - coarse.astype(jnp.float32)).astype(jnp.bfloat16)
        both = jnp.where(row_index < group, coarse.astype(jnp.float32), fine.astype(jnp.float32)).astype(jnp.bfloat16)
        mixes[slot] = jnp.dot(both, value_ref[0, 0, rows, :], preferred_element_type=jnp.float32)
        totals[slot] = jnp.broadcast_to(jnp.sum(spread, axis=-1, keepdims=True), (2 * group, HD))
        return carry

    lax.fori_loop(0, n, read_block, 0)

    def fold(j, carry):
        mixture, beyond = carry
        slot = n - 1 - j
        return mixture + jnp.exp(-beyond) * mixes[slot], beyond + totals[slot]

    zeros = jnp.zeros((2 * group, HD), jnp.float32)
    mixture, _ = lax.fori_loop(0, n, fold, (zeros, zeros))
    mixture = mixture[:group] + mixture[group:]
    mixture = mixture * lax.rsqrt(jnp.mean(mixture * mixture, axis=-1, keepdims=True) + EPSILON)
    read_ref[0] = jnp.concatenate([mixture[g : g + 1] for g in range(group)], axis=1).astype(jnp.bfloat16)

    def finish(j, carry):
        slot = lax.rem(me + j, n)

        @pl.when(j > 0)
        def _():
            off_copy(slot, slot).wait_send()
            for kv in range(2):
                block_copy(kv, slot, slot).wait_send()

        return carry

    lax.fori_loop(0, n, finish, 0)


def store_kernel(key_ref, value_ref, off_ref, read_ref, key_out, value_out, off_out, read_out, sems):
    copies = [
        pltpu.make_async_copy(source, target, sems.at[k])
        for k, (source, target) in enumerate(
            ((key_ref, key_out), (value_ref, value_out), (off_ref, off_out), (read_ref, read_out))
        )
    ]
    for copy in copies:
        copy.start()
    for copy in copies:
        copy.wait()


def shards(layer_input, input_gain, key_weight, value_weight, stick_offsets, head_bias, queries):
    seq_count, block, width = layer_input.shape
    n = lax.axis_size("sp")
    length = n * block
    group = H // KVH
    hbm = pl.BlockSpec(memory_space=pl.ANY)
    vmem = pl.BlockSpec(memory_space=pltpu.VMEM)
    smem = pl.BlockSpec(memory_space=pltpu.SMEM)
    shapes = ((1, 1, length, HD), (1, 1, length, HD), (1, 1, length), (1, 1, group * HD))
    arrived = pl.pallas_call(
        functools.partial(kernel, n),
        out_shape=tuple(pltpu.VMEM(shape, jnp.bfloat16) for shape in shapes),
        in_specs=[hbm] * 7,
        out_specs=(vmem, vmem, vmem, vmem),
        scratch_shapes=[
            pltpu.VMEM((1, width), jnp.float32),
            pltpu.VMEM(stick_offsets.shape, jnp.bfloat16),
            pltpu.SMEM(head_bias.shape, jnp.float32),
            pltpu.VMEM(queries.shape, jnp.bfloat16),
            pltpu.SemaphoreType.DMA((4,)),
            pltpu.VMEM((seq_count, block, width), jnp.bfloat16),
            pltpu.VMEM((KVH, width, 2 * HD), jnp.bfloat16),
            pltpu.VMEM((KVH, width, 2 * HD), jnp.bfloat16),
            pltpu.VMEM((width, HD), jnp.float32),
            pltpu.VMEM((block, HD), jnp.float32),
            pltpu.VMEM((n, 2, block, HD), jnp.bfloat16),
            pltpu.VMEM((n, 4, HD), jnp.bfloat16),
            pltpu.VMEM((n, 4, HD), jnp.bfloat16),
            pltpu.VMEM((block, block), jnp.bfloat16),
            pltpu.VMEM((n, 2 * group, HD), jnp.float32),
            pltpu.VMEM((n, 2 * group, HD), jnp.float32),
            pltpu.SemaphoreType.DMA((seq_count,)),
            pltpu.SemaphoreType.DMA((KVH, 2)),
            pltpu.SemaphoreType.DMA((n, 2)),
            pltpu.SemaphoreType.DMA((n, 2)),
            pltpu.SemaphoreType.DMA((n,)),
            pltpu.SemaphoreType.DMA((n,)),
            pltpu.SemaphoreType.REGULAR((n,)),
        ],
        compiler_params=pltpu.CompilerParams(collective_id=0, has_side_effects=True, vmem_limit_bytes=VMEM_LIMIT),
    )(
        *(
            pltpu.with_memory_space_constraint(array, pltpu.HBM)
            for array in (layer_input, input_gain.reshape(1, width), key_weight, value_weight, stick_offsets, head_bias, queries)
        )
    )
    return pl.pallas_call(
        store_kernel,
        out_shape=tuple(jax.ShapeDtypeStruct(shape, jnp.bfloat16) for shape in shapes),
        in_specs=[vmem] * 4,
        out_specs=(hbm,) * 4,
        scratch_shapes=[pltpu.SemaphoreType.DMA((4,))],
        compiler_params=pltpu.CompilerParams(vmem_limit_bytes=2**20),
    )(*arrived)


def solution(mesh):
    placed = (
        P(("grp", "tp"), "sp", None),
        P(),
        P(),
        P(),
        P(None, ("grp", "tp"), "sp"),
        P(),
        P(("grp", "tp"), "sp", None),
    )
    return jax.shard_map(
        shards,
        mesh=mesh,
        in_specs=placed,
        out_specs=(
            P(("grp", "tp"), "sp", None, None),
            P(("grp", "tp"), "sp", None, None),
            P(("grp", "tp"), "sp", None),
            P(("grp", "tp"), "sp", None),
        ),
        check_vma=False,
    )
```

```python
import functools
import math

import jax
import jax.numpy as jnp
from jax import lax
from jax.experimental import pallas as pl
from jax.experimental.pallas import tpu as pltpu
from jax.sharding import PartitionSpec as P

H = 16
KVH = 4
HD = 128
EPSILON = 1e-06
MESH = pl.DeviceIdType.MESH
TIE_TURN = 11
VMEM_LIMIT = 40 * 2**20


def split_rows(row, count):
    return [row[:, k * HD : (k + 1) * HD] for k in range(count)]


def kernel(
    n,
    x_ref, gain_hbm, wk_ref, wv_ref, off_hbm, bias_hbm, q_hbm,
    key_ref, value_ref, off_out_ref, read_ref,
    gain_ref, off_ref, bias_ref, q_ref, small_sem, x_buf, w_in, w_buf, gain_rows, scales, sent, relayed, off_sent, off_held, later, mixes, totals,
    x_sem, w_sem, send_sem, recv_sem, off_send_sem, off_recv_sem, relay_send_sem, relay_recv_sem, ready,
):
    prompts, block, width = x_ref.shape
    group = H // KVH
    lane_rows = block // HD
    me = lax.axis_index("sp")
    barrier = pltpu.get_barrier_semaphore()

    def x_copy(i):
        return pltpu.make_async_copy(x_ref.at[i], x_buf.at[i], x_sem.at[i])

    def w_copies(h):
        columns = pl.ds(h * HD, HD)
        return (
            pltpu.make_async_copy(wk_ref.at[:, columns], w_in.at[h, :, pl.ds(0, HD)], w_sem.at[h, 0]),
            pltpu.make_async_copy(wv_ref.at[:, columns], w_in.at[h, :, pl.ds(HD, HD)], w_sem.at[h, 1]),
        )

    small = [
        pltpu.make_async_copy(source, target, small_sem.at[k])
        for k, (source, target) in enumerate(
            ((off_hbm, off_ref), (gain_hbm, gain_ref), (bias_hbm, bias_ref), (q_hbm, q_ref))
        )
    ]
    x_copy(0).start()
    for copy in small:
        copy.start()
    for h in range(KVH):
        for copy in w_copies(h):
            copy.start()
    for i in range(1, prompts):
        x_copy(i).start()

    @pl.when(me > 0)
    def _():
        pl.semaphore_wait(barrier, 1)

    @pl.when(me < n - 1)
    def _():
        pl.semaphore_signal(barrier, inc=1, device_id={"sp": lax.rem(me + 1, n)}, device_id_type=MESH)

    def announce(t, carry):
        pl.semaphore_signal(ready.at[me], inc=1, device_id={"sp": t}, device_id_type=MESH)
        return carry

    lax.fori_loop(0, me, announce, 0)

    for copy in small:
        copy.wait()
    for k in range(width // HD):
        columns = jnp.broadcast_to(gain_ref[:, k * HD : (k + 1) * HD], (HD, HD))
        gain_rows[k * HD : (k + 1) * HD, :] = columns.T
    half, quarter = n // 2, n // 4
    by_relay, relays = me == half, me == quarter
    caches = (key_ref, value_ref)

    def place(kv, slot):
        return caches[kv].at[0, 0, pl.ds(pl.multiple_of(slot * block, block), block), :]

    def block_copy(kv, t, slot):
        return pltpu.make_async_remote_copy(
            sent.at[t, kv], place(kv, slot), send_sem.at[t, kv], recv_sem.at[slot, kv], device_id={"sp": t}, device_id_type=MESH
        )

    def off_copy(t, slot):
        return pltpu.make_async_remote_copy(
            off_sent.at[t], off_held.at[slot], off_send_sem.at[t], off_recv_sem.at[slot], device_id={"sp": t}, device_id_type=MESH
        )

    def to_relay(kv):
        return pltpu.make_async_remote_copy(
            sent.at[0, kv], relayed.at[kv], send_sem.at[0, kv], relay_recv_sem.at[kv],
            device_id={"sp": quarter}, device_id_type=MESH,
        )

    def from_relay(kv):
        return pltpu.make_async_remote_copy(
            relayed.at[kv], place(kv, half), relay_send_sem.at[kv], recv_sem.at[half, kv],
            device_id={"sp": 0}, device_id_type=MESH,
        )

    def send(t):
        through = jnp.logical_and(by_relay, t == 0)

        @pl.when(through)
        def _():
            for kv in range(2):
                to_relay(kv).start()

        @pl.when(jnp.logical_not(through))
        def _():
            for kv in range(2):
                block_copy(kv, t, me).start()

    def fold_gain(h):
        for kv in range(2):
            columns = pl.ds(kv * HD, HD)
            w_buf[h, :, columns] = (w_in[h, :, columns].astype(jnp.float32) * gain_rows[...]).astype(jnp.bfloat16)

    def measure_rows(i, start, count):
        rows = pl.ds(start, count)
        squares = jnp.zeros((count, HD), jnp.float32)
        for k in range(width // HD):
            x = x_buf[i, rows, pl.ds(k * HD, HD)].astype(jnp.float32)
            squares += x * x
        mean = jnp.sum(squares, axis=-1, keepdims=True) * (1.0 / width)
        scales[lax.rem(i, 2), rows, :] = jnp.broadcast_to(lax.rsqrt(mean + EPSILON), (count, HD))

    def project_pair(i, pair):
        for h in (2 * pair, 2 * pair + 1):
            rows = jnp.dot(x_buf[i], w_buf[h], preferred_element_type=jnp.float32)
            scale = scales[lax.rem(i, 2)]
            for kv in range(2):
                sent[i * KVH + h, kv] = (rows[:, kv * HD : (kv + 1) * HD] * scale).astype(jnp.bfloat16)

    def hand_out(i, pair):
        for h in (2 * pair, 2 * pair + 1):
            t = i * KVH + h

            @pl.when(t == me)
            def _():
                own = pl.ds(pl.multiple_of(me * block, block), block)
                for kv in range(2):
                    caches[kv][0, 0, own, :] = sent[t, kv]

            @pl.when(t < me)
            def _():
                send(t)

    for h in range(KVH):
        rows = off_ref[h].astype(jnp.float32)
        for i in range(prompts):
            pieces = split_rows(rows[i : i + 1], lane_rows)
            off_sent[i * KVH + h] = jnp.concatenate(pieces + pieces[:1], axis=0).astype(jnp.bfloat16)

    off_held[me] = off_sent[me]

    def send_offsets(t, carry):
        off_copy(t, me).start()
        return carry

    lax.fori_loop(0, me, send_offsets, 0)

    half_block = block // 2
    for h in range(2):
        for copy in w_copies(h):
            copy.wait()
        fold_gain(h)
    x_copy(0).wait()
    for k in range(2):
        measure_rows(0, k * half_block, half_block)

    def project_prompt(i, first):
        following = min(i + 1, prompts - 1) if first else jnp.minimum(i + 1, prompts - 1)
        for pair in range(KVH // 2):
            if first and pair == 0:
                for h in range(2, KVH):
                    for copy in w_copies(h):
                        copy.wait()
                    fold_gain(h)
                x_copy(1).wait()
            elif not first and pair == 0:

                @pl.when(i < prompts - 1)
                def _():
                    x_copy(i + 1).wait()

            project_pair(i, pair)
            measure_rows(following, pair * half_block, half_block)
            hand_out(i, pair)

    project_prompt(0, True)

    def project_rest(i, carry):
        project_prompt(i, False)
        return carry

    lax.fori_loop(1, prompts, project_rest, 0)

    def send_later(t, carry):
        pl.semaphore_wait(ready.at[t], 1)
        off_copy(t, me).start()
        send(t)

        @pl.when(jnp.logical_and(relays, t == n - quarter))
        def _():
            for kv in range(2):
                to_relay(kv).wait_recv()
                from_relay(kv).start()

        return carry

    lax.fori_loop(me + 1, n, send_later, 0)

    below = lax.broadcasted_iota(jnp.int32, (block, block), 0)
    across = lax.broadcasted_iota(jnp.int32, (block, block), 1)
    later[...] = jnp.where(below > across, 1.0, 0.0).astype(jnp.bfloat16)

    head = lax.rem(me, KVH)
    row_index = lax.broadcasted_iota(jnp.int32, (2 * group, 1), 0)
    query_rows = split_rows(q_ref[0], group)
    query = jnp.concatenate(query_rows + query_rows, axis=0)
    bias = jnp.zeros((2 * group, 1), jnp.float32)
    for g in range(group):
        bias = jnp.where(lax.rem(row_index, group) == g, bias_ref[head * group + g], bias)

    def source(j):
        k = jnp.where(j > TIE_TURN, j - 2, j - 1)
        away = jnp.where(lax.rem(k, 2) == 0, half - 1 - k // 2, n - 1 - k // 2)
        away = jnp.where(j == TIE_TURN, half, away)
        return lax.rem(me + jnp.where(j == 0, 0, away), n)

    def read_block(j, carry):
        slot = source(j)

        @pl.when(j > 0)
        def _():
            off_copy(slot, slot).wait_recv()
            for kv in range(2):
                block_copy(kv, slot, slot).wait_recv()

        rows = pl.ds(pl.multiple_of(slot * block, block), block)
        off_rows = off_held[slot].astype(jnp.float32)
        off_row = jnp.concatenate([off_rows[k : k + 1] for k in range(lane_rows)], axis=1)
        off_out_ref[0, :, pl.ds(pl.multiple_of(slot * block, HD), block)] = off_row.astype(jnp.bfloat16)
        scores = lax.dot_general(query, key_ref[0, 0, rows, :], (((1,), (1,)), ((), ())), preferred_element_type=jnp.float32)
        scores = scores * (1.0 / math.sqrt(HD)) + bias + off_row
        tail = jnp.log1p(jnp.exp(-jnp.abs(scores)))
        spread = jnp.maximum(scores, 0.0) + tail
        log_take = jnp.minimum(scores, 0.0) - tail
        high = spread.astype(jnp.bfloat16)
        rest = spread - high.astype(jnp.float32)
        middle = rest.astype(jnp.bfloat16)
        low = (rest - middle.astype(jnp.float32)).astype(jnp.bfloat16)
        parts = jnp.concatenate([part.astype(jnp.float32) for part in (high, middle, low)], axis=0).astype(jnp.bfloat16)
        sums = jnp.dot(parts, later[...], preferred_element_type=jnp.float32)
        inside = sums[: 2 * group] + sums[2 * group : 4 * group] + sums[4 * group :]
        weights = jnp.exp(log_take - inside)
        coarse = weights.astype(jnp.bfloat16)
        fine = (weights - coarse.astype(jnp.float32)).astype(jnp.bfloat16)
        both = jnp.where(row_index < group, coarse.astype(jnp.float32), fine.astype(jnp.float32)).astype(jnp.bfloat16)
        mixes[slot] = jnp.dot(both, value_ref[0, 0, rows, :], preferred_element_type=jnp.float32)
        totals[slot] = jnp.broadcast_to(jnp.sum(spread, axis=-1, keepdims=True), (2 * group, HD))
        return carry

    lax.fori_loop(0, n, read_block, 0)

    def fold(j, carry):
        mixture, beyond = carry
        slot = n - 1 - j
        return mixture + jnp.exp(-beyond) * mixes[slot], beyond + totals[slot]

    zeros = jnp.zeros((2 * group, HD), jnp.float32)
    mixture, _ = lax.fori_loop(0, n, fold, (zeros, zeros))
    mixture = mixture[:group] + mixture[group:]
    mixture = mixture * lax.rsqrt(jnp.mean(mixture * mixture, axis=-1, keepdims=True) + EPSILON)
    read_ref[0] = jnp.concatenate([mixture[g : g + 1] for g in range(group)], axis=1).astype(jnp.bfloat16)

    def finish(j, carry):
        slot = lax.rem(me + j, n)

        @pl.when(j > 0)
        def _():
            off_copy(slot, slot).wait_send()
            for kv in range(2):
                block_copy(kv, slot, slot).wait_send()

        return carry

    lax.fori_loop(0, n, finish, 0)

    @pl.when(relays)
    def _():
        for kv in range(2):
            from_relay(kv).wait_send()


def store_kernel(key_ref, value_ref, off_ref, read_ref, key_out, value_out, off_out, read_out, sems):
    copies = [
        pltpu.make_async_copy(source, target, sems.at[k])
        for k, (source, target) in enumerate(
            ((key_ref, key_out), (value_ref, value_out), (off_ref, off_out), (read_ref, read_out))
        )
    ]
    for copy in copies:
        copy.start()
    for copy in copies:
        copy.wait()


def shards(layer_input, input_gain, key_weight, value_weight, stick_offsets, head_bias, queries):
    seq_count, block, width = layer_input.shape
    n = lax.axis_size("sp")
    length = n * block
    group = H // KVH
    hbm = pl.BlockSpec(memory_space=pl.ANY)
    vmem = pl.BlockSpec(memory_space=pltpu.VMEM)
    smem = pl.BlockSpec(memory_space=pltpu.SMEM)
    shapes = ((1, 1, length, HD), (1, 1, length, HD), (1, 1, length), (1, 1, group * HD))
    arrived = pl.pallas_call(
        functools.partial(kernel, n),
        out_shape=tuple(pltpu.VMEM(shape, jnp.bfloat16) for shape in shapes),
        in_specs=[hbm] * 7,
        out_specs=(vmem, vmem, vmem, vmem),
        scratch_shapes=[
            pltpu.VMEM((1, width), jnp.float32),
            pltpu.VMEM(stick_offsets.shape, jnp.bfloat16),
            pltpu.SMEM(head_bias.shape, jnp.float32),
            pltpu.VMEM(queries.shape, jnp.bfloat16),
            pltpu.SemaphoreType.DMA((4,)),
            pltpu.VMEM((seq_count, block, width), jnp.bfloat16),
            pltpu.VMEM((KVH, width, 2 * HD), jnp.bfloat16),
            pltpu.VMEM((KVH, width, 2 * HD), jnp.bfloat16),
            pltpu.VMEM((width, HD), jnp.float32),
            pltpu.VMEM((2, block, HD), jnp.float32),
            pltpu.VMEM((n, 2, block, HD), jnp.bfloat16),
            pltpu.VMEM((2, block, HD), jnp.bfloat16),
            pltpu.VMEM((n, 4, HD), jnp.bfloat16),
            pltpu.VMEM((n, 4, HD), jnp.bfloat16),
            pltpu.VMEM((block, block), jnp.bfloat16),
            pltpu.VMEM((n, 2 * group, HD), jnp.float32),
            pltpu.VMEM((n, 2 * group, HD), jnp.float32),
            pltpu.SemaphoreType.DMA((seq_count,)),
            pltpu.SemaphoreType.DMA((KVH, 2)),
            pltpu.SemaphoreType.DMA((n, 2)),
            pltpu.SemaphoreType.DMA((n, 2)),
            pltpu.SemaphoreType.DMA((n,)),
            pltpu.SemaphoreType.DMA((n,)),
            pltpu.SemaphoreType.DMA((2,)),
            pltpu.SemaphoreType.DMA((2,)),
            pltpu.SemaphoreType.REGULAR((n,)),
        ],
        compiler_params=pltpu.CompilerParams(collective_id=0, has_side_effects=True, vmem_limit_bytes=VMEM_LIMIT),
    )(
        *(
            pltpu.with_memory_space_constraint(array, pltpu.HBM)
            for array in (layer_input, input_gain.reshape(1, width), key_weight, value_weight, stick_offsets, head_bias, queries)
        )
    )
    return pl.pallas_call(
        store_kernel,
        out_shape=tuple(jax.ShapeDtypeStruct(shape, jnp.bfloat16) for shape in shapes),
        in_specs=[vmem] * 4,
        out_specs=(hbm,) * 4,
        scratch_shapes=[pltpu.SemaphoreType.DMA((4,))],
        compiler_params=pltpu.CompilerParams(vmem_limit_bytes=2**20),
    )(*arrived)


def solution(mesh):
    placed = (
        P(("grp", "tp"), "sp", None),
        P(),
        P(),
        P(),
        P(None, ("grp", "tp"), "sp"),
        P(),
        P(("grp", "tp"), "sp", None),
    )
    return jax.shard_map(
        shards,
        mesh=mesh,
        in_specs=placed,
        out_specs=(
            P(("grp", "tp"), "sp", None, None),
            P(("grp", "tp"), "sp", None, None),
            P(("grp", "tp"), "sp", None),
            P(("grp", "tp"), "sp", None),
        ),
        check_vma=False,
    )
```

```python
import functools
import math

import jax
import jax.numpy as jnp
from jax import lax
from jax.experimental import pallas as pl
from jax.experimental.pallas import tpu as pltpu
from jax.sharding import PartitionSpec as P

H = 16
KVH = 4
HD = 128
EPSILON = 1e-06
MESH = pl.DeviceIdType.MESH
TIE_TURN = 11
STORES = 4
VMEM_LIMIT = 40 * 2**20


def split_rows(row, count):
    return [row[:, k * HD : (k + 1) * HD] for k in range(count)]


def kernel(
    n,
    x_ref, gain_hbm, wk_ref, wv_ref, off_hbm, bias_hbm, q_hbm,
    key_ref, value_ref, off_out_ref, read_ref,
    gain_ref, off_ref, bias_ref, q_ref, small_sem, x_buf, w_in, w_buf, gain_rows, scales, sent, relayed, off_sent, off_held, later, mixes, totals,
    x_sem, w_sem, send_sem, recv_sem, off_send_sem, off_recv_sem, relay_send_sem, relay_recv_sem, ready,
):
    prompts, block, width = x_ref.shape
    group = H // KVH
    lane_rows = block // HD
    me = lax.axis_index("sp")
    barrier = pltpu.get_barrier_semaphore()

    def x_copy(i):
        return pltpu.make_async_copy(x_ref.at[i], x_buf.at[i], x_sem.at[i])

    def w_copies(h):
        columns = pl.ds(h * HD, HD)
        return (
            pltpu.make_async_copy(wk_ref.at[:, columns], w_in.at[h, :, pl.ds(0, HD)], w_sem.at[h, 0]),
            pltpu.make_async_copy(wv_ref.at[:, columns], w_in.at[h, :, pl.ds(HD, HD)], w_sem.at[h, 1]),
        )

    small = [
        pltpu.make_async_copy(source, target, small_sem.at[k])
        for k, (source, target) in enumerate(
            ((off_hbm, off_ref), (gain_hbm, gain_ref), (bias_hbm, bias_ref), (q_hbm, q_ref))
        )
    ]
    x_copy(0).start()
    for copy in small:
        copy.start()
    for h in range(KVH):
        for copy in w_copies(h):
            copy.start()
    for i in range(1, prompts):
        x_copy(i).start()

    @pl.when(me > 0)
    def _():
        pl.semaphore_wait(barrier, 1)

    @pl.when(me < n - 1)
    def _():
        pl.semaphore_signal(barrier, inc=1, device_id={"sp": lax.rem(me + 1, n)}, device_id_type=MESH)

    def announce(t, carry):
        pl.semaphore_signal(ready.at[me], inc=1, device_id={"sp": t}, device_id_type=MESH)
        return carry

    lax.fori_loop(0, me, announce, 0)

    for copy in small:
        copy.wait()
    for k in range(width // HD):
        columns = jnp.broadcast_to(gain_ref[:, k * HD : (k + 1) * HD], (HD, HD))
        gain_rows[k * HD : (k + 1) * HD, :] = columns.T
    half, quarter = n // 2, n // 4
    by_relay, relays = me == half, me == quarter
    caches = (key_ref, value_ref)

    def place(kv, slot):
        return caches[kv].at[0, 0, pl.ds(pl.multiple_of(slot * block, block), block), :]

    def block_copy(kv, t, slot):
        return pltpu.make_async_remote_copy(
            sent.at[t, kv], place(kv, slot), send_sem.at[t, kv], recv_sem.at[slot, kv], device_id={"sp": t}, device_id_type=MESH
        )

    def off_copy(t, slot):
        return pltpu.make_async_remote_copy(
            off_sent.at[t], off_held.at[slot], off_send_sem.at[t], off_recv_sem.at[slot], device_id={"sp": t}, device_id_type=MESH
        )

    def to_relay(kv):
        return pltpu.make_async_remote_copy(
            sent.at[0, kv], relayed.at[kv], send_sem.at[0, kv], relay_recv_sem.at[kv],
            device_id={"sp": quarter}, device_id_type=MESH,
        )

    def from_relay(kv):
        return pltpu.make_async_remote_copy(
            relayed.at[kv], place(kv, half), relay_send_sem.at[kv], recv_sem.at[half, kv],
            device_id={"sp": 0}, device_id_type=MESH,
        )

    def send(t):
        through = jnp.logical_and(by_relay, t == 0)

        @pl.when(through)
        def _():
            for kv in range(2):
                to_relay(kv).start()

        @pl.when(jnp.logical_not(through))
        def _():
            for kv in range(2):
                block_copy(kv, t, me).start()

    def fold_gain(h):
        for kv in range(2):
            columns = pl.ds(kv * HD, HD)
            w_buf[h, :, columns] = (w_in[h, :, columns].astype(jnp.float32) * gain_rows[...]).astype(jnp.bfloat16)

    def measure_rows(i, start, count):
        rows = pl.ds(start, count)
        squares = jnp.zeros((count, HD), jnp.float32)
        for k in range(width // HD):
            x = x_buf[i, rows, pl.ds(k * HD, HD)].astype(jnp.float32)
            squares += x * x
        mean = jnp.sum(squares, axis=-1, keepdims=True) * (1.0 / width)
        scales[lax.rem(i, 2), rows, :] = jnp.broadcast_to(lax.rsqrt(mean + EPSILON), (count, HD))

    def project_heads(i, heads):
        for h in heads:
            rows = jnp.dot(x_buf[i], w_buf[h], preferred_element_type=jnp.float32)
            scale = scales[lax.rem(i, 2)]
            for kv in range(2):
                sent[i * KVH + h, kv] = (rows[:, kv * HD : (kv + 1) * HD] * scale).astype(jnp.bfloat16)

    def hand_out(i, heads):
        for h in heads:
            t = i * KVH + h

            @pl.when(t == me)
            def _():
                own = pl.ds(pl.multiple_of(me * block, block), block)
                for kv in range(2):
                    caches[kv][0, 0, own, :] = sent[t, kv]

            @pl.when(t > me)
            def _():
                pl.semaphore_wait(ready.at[t], 1)
                off_copy(t, me).start()

            @pl.when(t != me)
            def _():
                send(t)

            @pl.when(jnp.logical_and(relays, t == n - quarter))
            def _():
                for kv in range(2):
                    to_relay(kv).wait_recv()
                    from_relay(kv).start()

    half_block = block // 2

    def wait_weights(h):
        for copy in w_copies(h):
            copy.wait()

    wait_weights(0)
    fold_gain(0)
    wait_weights(1)
    x_copy(0).wait()
    for k in range(2):
        measure_rows(0, k * half_block, half_block)
    project_heads(0, (0,))
    fold_gain(1)
    hand_out(0, (0,))

    for h in range(KVH):
        rows = off_ref[h].astype(jnp.float32)
        for i in range(prompts):
            pieces = split_rows(rows[i : i + 1], lane_rows)
            off_sent[i * KVH + h] = jnp.concatenate(pieces + pieces[:1], axis=0).astype(jnp.bfloat16)

    off_held[me] = off_sent[me]

    def send_offsets(t, carry):
        off_copy(t, me).start()
        return carry

    lax.fori_loop(0, me, send_offsets, 0)

    wait_weights(2)
    wait_weights(3)
    project_heads(0, (1,))
    fold_gain(2)
    fold_gain(3)
    hand_out(0, (1,))
    x_copy(1).wait()
    project_heads(0, (2, 3))
    for k in range(2):
        measure_rows(1, k * half_block, half_block)
    hand_out(0, (2, 3))

    def project_prompt(i):
        following = jnp.minimum(i + 1, prompts - 1)

        @pl.when(i < prompts - 1)
        def _():
            x_copy(i + 1).wait()

        for pair in range(KVH // 2):
            heads = (2 * pair, 2 * pair + 1)
            project_heads(i, heads)
            measure_rows(following, pair * half_block, half_block)
            hand_out(i, heads)

    def project_rest(i, carry):
        project_prompt(i)
        return carry

    lax.fori_loop(1, prompts, project_rest, 0)

    below = lax.broadcasted_iota(jnp.int32, (block, block), 0)
    across = lax.broadcasted_iota(jnp.int32, (block, block), 1)
    later[...] = jnp.where(below > across, 1.0, 0.0).astype(jnp.bfloat16)

    head = lax.rem(me, KVH)
    row_index = lax.broadcasted_iota(jnp.int32, (2 * group, 1), 0)
    query_rows = split_rows(q_ref[0], group)
    query = jnp.concatenate(query_rows + query_rows, axis=0)
    bias = jnp.zeros((2 * group, 1), jnp.float32)
    for g in range(group):
        bias = jnp.where(lax.rem(row_index, group) == g, bias_ref[head * group + g], bias)

    def source(j):
        k = jnp.where(j > TIE_TURN, j - 2, j - 1)
        away = jnp.where(lax.rem(k, 2) == 0, half - 1 - k // 2, n - 1 - k // 2)
        away = jnp.where(j == TIE_TURN, half, away)
        return lax.rem(me + jnp.where(j == 0, 0, away), n)

    def read_block(j, carry):
        slot = source(j)

        @pl.when(j > 0)
        def _():
            off_copy(slot, slot).wait_recv()
            for kv in range(2):
                block_copy(kv, slot, slot).wait_recv()

        rows = pl.ds(pl.multiple_of(slot * block, block), block)
        off_rows = off_held[slot].astype(jnp.float32)
        off_row = jnp.concatenate([off_rows[k : k + 1] for k in range(lane_rows)], axis=1)
        off_out_ref[0, :, pl.ds(pl.multiple_of(slot * block, HD), block)] = off_row.astype(jnp.bfloat16)
        scores = lax.dot_general(query, key_ref[0, 0, rows, :], (((1,), (1,)), ((), ())), preferred_element_type=jnp.float32)
        scores = scores * (1.0 / math.sqrt(HD)) + bias + off_row
        tail = jnp.log1p(jnp.exp(-jnp.abs(scores)))
        spread = jnp.maximum(scores, 0.0) + tail
        log_take = jnp.minimum(scores, 0.0) - tail
        high = spread.astype(jnp.bfloat16)
        rest = spread - high.astype(jnp.float32)
        middle = rest.astype(jnp.bfloat16)
        low = (rest - middle.astype(jnp.float32)).astype(jnp.bfloat16)
        parts = jnp.concatenate([part.astype(jnp.float32) for part in (high, middle, low)], axis=0).astype(jnp.bfloat16)
        sums = jnp.dot(parts, later[...], preferred_element_type=jnp.float32)
        inside = sums[: 2 * group] + sums[2 * group : 4 * group] + sums[4 * group :]
        weights = jnp.exp(log_take - inside)
        coarse = weights.astype(jnp.bfloat16)
        fine = (weights - coarse.astype(jnp.float32)).astype(jnp.bfloat16)
        both = jnp.where(row_index < group, coarse.astype(jnp.float32), fine.astype(jnp.float32)).astype(jnp.bfloat16)
        mixes[slot] = jnp.dot(both, value_ref[0, 0, rows, :], preferred_element_type=jnp.float32)
        totals[slot] = jnp.broadcast_to(jnp.sum(spread, axis=-1, keepdims=True), (2 * group, HD))
        return carry

    lax.fori_loop(0, n, read_block, 0)

    def fold(j, carry):
        mixture, beyond = carry
        slot = n - 1 - j
        return mixture + jnp.exp(-beyond) * mixes[slot], beyond + totals[slot]

    zeros = jnp.zeros((2 * group, HD), jnp.float32)
    mixture, _ = lax.fori_loop(0, n, fold, (zeros, zeros), unroll=True)
    mixture = mixture[:group] + mixture[group:]
    mixture = mixture * lax.rsqrt(jnp.mean(mixture * mixture, axis=-1, keepdims=True) + EPSILON)
    read_ref[0] = jnp.concatenate([mixture[g : g + 1] for g in range(group)], axis=1).astype(jnp.bfloat16)

    def finish(j, carry):
        slot = lax.rem(me + j, n)

        @pl.when(j > 0)
        def _():
            off_copy(slot, slot).wait_send()
            for kv in range(2):
                block_copy(kv, slot, slot).wait_send()

        return carry

    lax.fori_loop(0, n, finish, 0)

    @pl.when(relays)
    def _():
        for kv in range(2):
            from_relay(kv).wait_send()


def store_kernel(key_ref, value_ref, off_ref, read_ref, key_out, value_out, off_out, read_out, sems):
    pairs = [(off_ref, off_out), (read_ref, read_out)]
    rows = key_ref.shape[2] // STORES
    for k in range(STORES):
        part = pl.ds(k * rows, rows)
        for source, target in ((key_ref, key_out), (value_ref, value_out)):
            pairs.append((source.at[0, 0, part, :], target.at[0, 0, part, :]))
    copies = [pltpu.make_async_copy(source, target, sems.at[k]) for k, (source, target) in enumerate(pairs)]
    for copy in copies:
        copy.start()
    for copy in copies:
        copy.wait()


def shards(layer_input, input_gain, key_weight, value_weight, stick_offsets, head_bias, queries):
    seq_count, block, width = layer_input.shape
    n = lax.axis_size("sp")
    length = n * block
    group = H // KVH
    hbm = pl.BlockSpec(memory_space=pl.ANY)
    vmem = pl.BlockSpec(memory_space=pltpu.VMEM)
    smem = pl.BlockSpec(memory_space=pltpu.SMEM)
    shapes = ((1, 1, length, HD), (1, 1, length, HD), (1, 1, length), (1, 1, group * HD))
    arrived = pl.pallas_call(
        functools.partial(kernel, n),
        out_shape=tuple(pltpu.VMEM(shape, jnp.bfloat16) for shape in shapes),
        in_specs=[hbm] * 7,
        out_specs=(vmem, vmem, vmem, vmem),
        scratch_shapes=[
            pltpu.VMEM((1, width), jnp.float32),
            pltpu.VMEM(stick_offsets.shape, jnp.bfloat16),
            pltpu.SMEM(head_bias.shape, jnp.float32),
            pltpu.VMEM(queries.shape, jnp.bfloat16),
            pltpu.SemaphoreType.DMA((4,)),
            pltpu.VMEM((seq_count, block, width), jnp.bfloat16),
            pltpu.VMEM((KVH, width, 2 * HD), jnp.bfloat16),
            pltpu.VMEM((KVH, width, 2 * HD), jnp.bfloat16),
            pltpu.VMEM((width, HD), jnp.float32),
            pltpu.VMEM((2, block, HD), jnp.float32),
            pltpu.VMEM((n, 2, block, HD), jnp.bfloat16),
            pltpu.VMEM((2, block, HD), jnp.bfloat16),
            pltpu.VMEM((n, 4, HD), jnp.bfloat16),
            pltpu.VMEM((n, 4, HD), jnp.bfloat16),
            pltpu.VMEM((block, block), jnp.bfloat16),
            pltpu.VMEM((n, 2 * group, HD), jnp.float32),
            pltpu.VMEM((n, 2 * group, HD), jnp.float32),
            pltpu.SemaphoreType.DMA((seq_count,)),
            pltpu.SemaphoreType.DMA((KVH, 2)),
            pltpu.SemaphoreType.DMA((n, 2)),
            pltpu.SemaphoreType.DMA((n, 2)),
            pltpu.SemaphoreType.DMA((n,)),
            pltpu.SemaphoreType.DMA((n,)),
            pltpu.SemaphoreType.DMA((2,)),
            pltpu.SemaphoreType.DMA((2,)),
            pltpu.SemaphoreType.REGULAR((n,)),
        ],
        compiler_params=pltpu.CompilerParams(collective_id=0, has_side_effects=True, vmem_limit_bytes=VMEM_LIMIT),
    )(
        *(
            pltpu.with_memory_space_constraint(array, pltpu.HBM)
            for array in (layer_input, input_gain.reshape(1, width), key_weight, value_weight, stick_offsets, head_bias, queries)
        )
    )
    return pl.pallas_call(
        store_kernel,
        out_shape=tuple(jax.ShapeDtypeStruct(shape, jnp.bfloat16) for shape in shapes),
        in_specs=[vmem] * 4,
        out_specs=(hbm,) * 4,
        scratch_shapes=[pltpu.SemaphoreType.DMA((2 * STORES + 2,))],
        compiler_params=pltpu.CompilerParams(vmem_limit_bytes=2**20),
    )(*arrived)


def solution(mesh):
    placed = (
        P(("grp", "tp"), "sp", None),
        P(),
        P(),
        P(),
        P(None, ("grp", "tp"), "sp"),
        P(),
        P(("grp", "tp"), "sp", None),
    )
    return jax.shard_map(
        shards,
        mesh=mesh,
        in_specs=placed,
        out_specs=(
            P(("grp", "tp"), "sp", None, None),
            P(("grp", "tp"), "sp", None, None),
            P(("grp", "tp"), "sp", None),
            P(("grp", "tp"), "sp", None),
        ),
        check_vma=False,
    )
```

```python
import functools
import math

import jax
import jax.numpy as jnp
from jax import lax
from jax.experimental import pallas as pl
from jax.experimental.pallas import tpu as pltpu
from jax.sharding import PartitionSpec as P

H = 16
KVH = 4
HD = 128
EPSILON = 1e-06
MESH = pl.DeviceIdType.MESH
TIE_TURN = 11
STORES = 4
VMEM_LIMIT = 40 * 2**20


def split_rows(row, count):
    return [row[:, k * HD : (k + 1) * HD] for k in range(count)]


def kernel(
    n,
    x_ref, gain_hbm, wk_ref, wv_ref, off_hbm, bias_hbm, q_hbm,
    held, off_out_ref, read_ref,
    gain_ref, off_ref, bias_ref, q_ref, small_sem, x_buf, w_in, w_buf, gain_rows, scales, sent, relayed, off_sent, off_held, later, mixes, totals,
    x_sem, w_sem, send_sem, recv_sem, off_send_sem, off_recv_sem, relay_sem, ready,
):
    prompts, block, width = x_ref.shape
    group = H // KVH
    lane_rows = block // HD
    me = lax.axis_index("sp")
    barrier = pltpu.get_barrier_semaphore()

    def x_copy(i):
        return pltpu.make_async_copy(x_ref.at[i], x_buf.at[i], x_sem.at[i])

    def w_copies(h):
        columns = pl.ds(h * HD, HD)
        return (
            pltpu.make_async_copy(wk_ref.at[:, columns], w_in.at[h, :, pl.ds(0, HD)], w_sem.at[h, 0]),
            pltpu.make_async_copy(wv_ref.at[:, columns], w_in.at[h, :, pl.ds(HD, HD)], w_sem.at[h, 1]),
        )

    small = [
        pltpu.make_async_copy(source, target, small_sem.at[k])
        for k, (source, target) in enumerate(
            ((off_hbm, off_ref), (gain_hbm, gain_ref), (bias_hbm, bias_ref), (q_hbm, q_ref))
        )
    ]
    for copy in small:
        copy.start()
    for copy in w_copies(0):
        copy.start()
    x_copy(0).start()

    @pl.when(me > 0)
    def _():
        pl.semaphore_wait(barrier, 1)

    @pl.when(me < n - 1)
    def _():
        pl.semaphore_signal(barrier, inc=1, device_id={"sp": lax.rem(me + 1, n)}, device_id_type=MESH)

    def announce(t, carry):
        pl.semaphore_signal(ready.at[me], inc=1, device_id={"sp": t}, device_id_type=MESH)
        return carry

    lax.fori_loop(0, me, announce, 0)

    for copy in small:
        copy.wait()
    for k in range(width // HD):
        columns = jnp.broadcast_to(gain_ref[:, k * HD : (k + 1) * HD], (HD, HD))
        gain_rows[k * HD : (k + 1) * HD, :] = columns.T
    half, quarter = n // 2, n // 4
    by_relay, relays = me == half, me == quarter
    def block_copy(t, slot):
        return pltpu.make_async_remote_copy(
            sent.at[t], held.at[slot], send_sem.at[t], recv_sem.at[slot], device_id={"sp": t}, device_id_type=MESH
        )

    def off_copy(t, slot):
        return pltpu.make_async_remote_copy(
            off_sent.at[t], off_held.at[slot], off_send_sem.at[t], off_recv_sem.at[slot], device_id={"sp": t}, device_id_type=MESH
        )

    def to_relay():
        return pltpu.make_async_remote_copy(
            sent.at[0], relayed, send_sem.at[0], relay_sem.at[0], device_id={"sp": quarter}, device_id_type=MESH
        )

    def from_relay():
        return pltpu.make_async_remote_copy(
            relayed, held.at[half], relay_sem.at[1], recv_sem.at[half], device_id={"sp": 0}, device_id_type=MESH
        )

    def send(t):
        through = jnp.logical_and(by_relay, t == 0)

        @pl.when(through)
        def _():
            to_relay().start()

        @pl.when(jnp.logical_not(through))
        def _():
            block_copy(t, me).start()

    def fold_gain(h):
        for kv in range(2):
            columns = pl.ds(kv * HD, HD)
            w_buf[h, :, columns] = (w_in[h, :, columns].astype(jnp.float32) * gain_rows[...]).astype(jnp.bfloat16)

    def measure_rows(i, start, count):
        rows = pl.ds(start, count)
        squares = jnp.zeros((count, HD), jnp.float32)
        for k in range(width // HD):
            x = x_buf[i, rows, pl.ds(k * HD, HD)].astype(jnp.float32)
            squares += x * x
        mean = jnp.sum(squares, axis=-1, keepdims=True) * (1.0 / width)
        scales[lax.rem(i, 2), rows, :] = jnp.broadcast_to(lax.rsqrt(mean + EPSILON), (count, HD))

    def project_heads(i, heads):
        for h in heads:
            rows = jnp.dot(x_buf[i], w_buf[h], preferred_element_type=jnp.float32)
            scale = scales[lax.rem(i, 2)]
            for kv in range(2):
                sent[i * KVH + h, kv] = (rows[:, kv * HD : (kv + 1) * HD] * scale).astype(jnp.bfloat16)

    def hand_out(i, heads):
        for h in heads:
            t = i * KVH + h

            @pl.when(t == me)
            def _():
                held[me] = sent[t]

            @pl.when(t > me)
            def _():
                pl.semaphore_wait(ready.at[t], 1)
                off_copy(t, me).start()

            behind = jnp.logical_and(jnp.logical_and(me > 0, me < half), t >= me + half)

            @pl.when(jnp.logical_and(t != me, jnp.logical_not(behind)))
            def _():
                send(t)

            @pl.when(jnp.logical_and(behind, t > me + half))
            def _():
                send(jnp.maximum(t - 1, 0))

            @pl.when(jnp.logical_and(behind, t == n - 1))
            def _():
                send(t)

            @pl.when(jnp.logical_and(relays, t == n - quarter))
            def _():
                to_relay().wait_recv()
                from_relay().start()

    half_block = block // 2

    def wait_weights(h):
        for copy in w_copies(h):
            copy.wait()

    wait_weights(0)
    for h in range(1, KVH):
        for copy in w_copies(h):
            copy.start()
    fold_gain(0)
    x_copy(0).wait()
    for i in range(1, prompts):
        x_copy(i).start()
    for k in range(2):
        measure_rows(0, k * half_block, half_block)
    project_heads(0, (0,))
    wait_weights(1)
    fold_gain(1)
    hand_out(0, (0,))

    for h in range(KVH):
        rows = off_ref[h].astype(jnp.float32)
        for i in range(prompts):
            pieces = split_rows(rows[i : i + 1], lane_rows)
            off_sent[i * KVH + h] = jnp.concatenate(pieces + pieces[:1], axis=0).astype(jnp.bfloat16)

    off_held[me] = off_sent[me]

    def send_offsets(t, carry):
        off_copy(t, me).start()
        return carry

    lax.fori_loop(0, me, send_offsets, 0)

    wait_weights(2)
    wait_weights(3)
    project_heads(0, (1,))
    fold_gain(2)
    fold_gain(3)
    hand_out(0, (1,))
    x_copy(1).wait()
    project_heads(0, (2, 3))
    for k in range(2):
        measure_rows(1, k * half_block, half_block)
    hand_out(0, (2, 3))

    def project_prompt(i):
        following = jnp.minimum(i + 1, prompts - 1)

        @pl.when(i < prompts - 1)
        def _():
            x_copy(i + 1).wait()

        for pair in range(KVH // 2):
            heads = (2 * pair, 2 * pair + 1)
            project_heads(i, heads)
            measure_rows(following, pair * half_block, half_block)
            hand_out(i, heads)

    def project_rest(i, carry):
        project_prompt(i)
        return carry

    lax.fori_loop(1, prompts, project_rest, 0)

    below = lax.broadcasted_iota(jnp.int32, (block, block), 0)
    across = lax.broadcasted_iota(jnp.int32, (block, block), 1)
    later[...] = jnp.where(below > across, 1.0, 0.0).astype(jnp.bfloat16)

    head = lax.rem(me, KVH)
    row_index = lax.broadcasted_iota(jnp.int32, (2 * group, 1), 0)
    query_rows = split_rows(q_ref[0], group)
    query = jnp.concatenate(query_rows + query_rows, axis=0)
    bias = jnp.zeros((2 * group, 1), jnp.float32)
    for g in range(group):
        bias = jnp.where(lax.rem(row_index, group) == g, bias_ref[head * group + g], bias)

    def source(j):
        k = jnp.where(j > TIE_TURN, j - 2, j - 1)
        away = jnp.where(lax.rem(k, 2) == 0, half - 1 - k // 2, n - 1 - k // 2)
        away = jnp.where(j == TIE_TURN, half, away)
        return lax.rem(me + jnp.where(j == 0, 0, away), n)

    def read_block(j, carry):
        slot = source(j)

        @pl.when(j > 0)
        def _():
            off_copy(slot, slot).wait_recv()
            block_copy(slot, slot).wait_recv()

        off_rows = off_held[slot].astype(jnp.float32)
        off_row = jnp.concatenate([off_rows[k : k + 1] for k in range(lane_rows)], axis=1)
        off_out_ref[0, :, pl.ds(pl.multiple_of(slot * block, HD), block)] = off_row.astype(jnp.bfloat16)
        scores = lax.dot_general(query, held[slot, 0], (((1,), (1,)), ((), ())), preferred_element_type=jnp.float32)
        scores = scores * (1.0 / math.sqrt(HD)) + bias + off_row
        tail = jnp.log1p(jnp.exp(-jnp.abs(scores)))
        spread = jnp.maximum(scores, 0.0) + tail
        log_take = jnp.minimum(scores, 0.0) - tail
        high = spread.astype(jnp.bfloat16)
        rest = spread - high.astype(jnp.float32)
        middle = rest.astype(jnp.bfloat16)
        low = (rest - middle.astype(jnp.float32)).astype(jnp.bfloat16)
        parts = jnp.concatenate([part.astype(jnp.float32) for part in (high, middle, low)], axis=0).astype(jnp.bfloat16)
        sums = jnp.dot(parts, later[...], preferred_element_type=jnp.float32)
        inside = sums[: 2 * group] + sums[2 * group : 4 * group] + sums[4 * group :]
        weights = jnp.exp(log_take - inside)
        coarse = weights.astype(jnp.bfloat16)
        fine = (weights - coarse.astype(jnp.float32)).astype(jnp.bfloat16)
        both = jnp.where(row_index < group, coarse.astype(jnp.float32), fine.astype(jnp.float32)).astype(jnp.bfloat16)
        mixes[slot] = jnp.dot(both, held[slot, 1], preferred_element_type=jnp.float32)
        totals[slot] = jnp.broadcast_to(jnp.sum(spread, axis=-1, keepdims=True), (2 * group, HD))
        return carry

    lax.fori_loop(0, n, read_block, 0)

    def fold(j, carry):
        mixture, beyond = carry
        slot = n - 1 - j
        return mixture + jnp.exp(-beyond) * mixes[slot], beyond + totals[slot]

    zeros = jnp.zeros((2 * group, HD), jnp.float32)
    mixture, _ = lax.fori_loop(0, n, fold, (zeros, zeros), unroll=True)
    mixture = mixture[:group] + mixture[group:]
    mixture = mixture * lax.rsqrt(jnp.mean(mixture * mixture, axis=-1, keepdims=True) + EPSILON)
    read_ref[0] = jnp.concatenate([mixture[g : g + 1] for g in range(group)], axis=1).astype(jnp.bfloat16)

    def finish(j, carry):
        slot = lax.rem(me + j, n)

        @pl.when(j > 0)
        def _():
            off_copy(slot, slot).wait_send()
            block_copy(slot, slot).wait_send()

        return carry

    lax.fori_loop(0, n, finish, 0)

    @pl.when(relays)
    def _():
        from_relay().wait_send()


def store_kernel(held, off_ref, read_ref, key_out, value_out, off_out, read_out, sems):
    pairs = [(off_ref, off_out), (read_ref, read_out)]
    blocks = held.shape[0] // STORES
    for k in range(STORES):
        part = pl.ds(k * blocks, blocks)
        for kv, target in enumerate((key_out, value_out)):
            pairs.append((held.at[part, kv], target.at[part]))
    copies = [pltpu.make_async_copy(source, target, sems.at[k]) for k, (source, target) in enumerate(pairs)]
    for copy in copies:
        copy.start()
    for copy in copies:
        copy.wait()


def shards(layer_input, input_gain, key_weight, value_weight, stick_offsets, head_bias, queries):
    seq_count, block, width = layer_input.shape
    n = lax.axis_size("sp")
    length = n * block
    group = H // KVH
    hbm = pl.BlockSpec(memory_space=pl.ANY)
    vmem = pl.BlockSpec(memory_space=pltpu.VMEM)
    smem = pl.BlockSpec(memory_space=pltpu.SMEM)
    small = ((1, 1, length), (1, 1, group * HD))
    shapes = ((n, block, HD), (n, block, HD)) + small
    arrived = pl.pallas_call(
        functools.partial(kernel, n),
        out_shape=tuple(pltpu.VMEM(shape, jnp.bfloat16) for shape in ((n, 2, block, HD),) + small),
        in_specs=[hbm] * 7,
        out_specs=(vmem, vmem, vmem),
        scratch_shapes=[
            pltpu.VMEM((1, width), jnp.float32),
            pltpu.VMEM(stick_offsets.shape, jnp.bfloat16),
            pltpu.SMEM(head_bias.shape, jnp.float32),
            pltpu.VMEM(queries.shape, jnp.bfloat16),
            pltpu.SemaphoreType.DMA((4,)),
            pltpu.VMEM((seq_count, block, width), jnp.bfloat16),
            pltpu.VMEM((KVH, width, 2 * HD), jnp.bfloat16),
            pltpu.VMEM((KVH, width, 2 * HD), jnp.bfloat16),
            pltpu.VMEM((width, HD), jnp.float32),
            pltpu.VMEM((2, block, HD), jnp.float32),
            pltpu.VMEM((n, 2, block, HD), jnp.bfloat16),
            pltpu.VMEM((2, block, HD), jnp.bfloat16),
            pltpu.VMEM((n, 4, HD), jnp.bfloat16),
            pltpu.VMEM((n, 4, HD), jnp.bfloat16),
            pltpu.VMEM((block, block), jnp.bfloat16),
            pltpu.VMEM((n, 2 * group, HD), jnp.float32),
            pltpu.VMEM((n, 2 * group, HD), jnp.float32),
            pltpu.SemaphoreType.DMA((seq_count,)),
            pltpu.SemaphoreType.DMA((KVH, 2)),
            pltpu.SemaphoreType.DMA((n,)),
            pltpu.SemaphoreType.DMA((n,)),
            pltpu.SemaphoreType.DMA((n,)),
            pltpu.SemaphoreType.DMA((n,)),
            pltpu.SemaphoreType.DMA((2,)),
            pltpu.SemaphoreType.REGULAR((n,)),
        ],
        compiler_params=pltpu.CompilerParams(collective_id=0, has_side_effects=True, vmem_limit_bytes=VMEM_LIMIT),
    )(
        *(
            pltpu.with_memory_space_constraint(array, pltpu.HBM)
            for array in (layer_input, input_gain.reshape(1, width), key_weight, value_weight, stick_offsets, head_bias, queries)
        )
    )
    keys, values, offsets, read = pl.pallas_call(
        store_kernel,
        out_shape=tuple(jax.ShapeDtypeStruct(shape, jnp.bfloat16) for shape in shapes),
        in_specs=[vmem] * 3,
        out_specs=(hbm,) * 4,
        scratch_shapes=[pltpu.SemaphoreType.DMA((2 * STORES + 2,))],
        compiler_params=pltpu.CompilerParams(vmem_limit_bytes=2**20),
    )(*arrived)
    return keys.reshape(1, 1, length, HD), values.reshape(1, 1, length, HD), offsets, read


def solution(mesh):
    placed = (
        P(("grp", "tp"), "sp", None),
        P(),
        P(),
        P(),
        P(None, ("grp", "tp"), "sp"),
        P(),
        P(("grp", "tp"), "sp", None),
    )
    return jax.shard_map(
        shards,
        mesh=mesh,
        in_specs=placed,
        out_specs=(
            P(("grp", "tp"), "sp", None, None),
            P(("grp", "tp"), "sp", None, None),
            P(("grp", "tp"), "sp", None),
            P(("grp", "tp"), "sp", None),
        ),
        check_vma=False,
    )
```
